256 devices in a mesh: fs: 16 (over y, x), tp: 16 (over z, core).
Axes of the slice: x: 4, y: 4, z: 8, core: 2. Of those that a mesh axis runs over, the one named last changes fastest.
Arguments:
- tokens: bfloat16 [16384, 2048], P(('fs', 'tp')), may hold values from -6 to 6
- gate_weight: bfloat16 [2048, 5632], P('fs', 'tp'), may hold values from -0.125 to 0.125
- up_weight: bfloat16 [2048, 5632], P('fs', 'tp'), may hold values from -0.125 to 0.125
- down_weight: bfloat16 [5632, 2048], P('tp', 'fs'), may hold values from -0.078125 to 0.078125
- grad_out: bfloat16 [16384, 2048], P(('fs', 'tp')), may hold values from -24 to 24
Outputs:
- grad_input: bfloat16 [16384, 2048], P(('fs', 'tp'))
- grad_gate: float32 [2048, 5632], P('fs', 'tp')
- grad_up: float32 [2048, 5632], P('fs', 'tp')
- grad_down: float32 [5632, 2048], P('tp', 'fs')
The draws below stay inside these ranges and needn't reach their ends.
All inputs are finite; a program needn't handle non-finite values.
Results may differ from the reference program's by a relative error of at most 0.0049.
Values may be sent and summed in bfloat16 or wider, within the bound.
No kernel may reach another device: no remote copies, remote signals or barrier semaphores. Data moves between devices by JAX's collectives and lax.ppermute only.
A program may use at most 128 MiB of HBM per device.

```python
import jax
import jax.numpy as jnp

D = 2048
FF = 5632
TOKENS = 16384


def spiked(array, key, source, target, parts, factor):
    owner, partner = [(jnp.arange(array.shape[dim]) // (array.shape[dim] // parts)).reshape([-1 if axis == dim else 1 for axis in range(array.ndim)]) for dim in (source, target)]
    chosen = jax.random.permutation(key, parts)[partner]
    strong = (owner == chosen) | (owner == (partner + parts // 2) % parts)
    return jnp.where(strong, factor * array, array)


def shard_levels(own_key, dims, shards, least, high):
    factor_of, own = 1.0, jax.random.fold_in(own_key, 6)
    for position, shards_of in shards:
        draws = jnp.exp(jax.random.uniform(jax.random.fold_in(own, position), (shards_of,), jnp.float32, least / len(shards), high / len(shards)))
        factor_of = factor_of * jnp.repeat(draws, dims[position] // shards_of).reshape([-1 if axis == position else 1 for axis in range(len(dims))])
    return factor_of


def bell_draw(own_key, dims, spread, limit, split=(), held_as=jnp.bfloat16):
    factor_of = shard_levels(own_key, dims, split, -0.22, 0.18) if split else 1.0
    result = jax.random.normal(own_key, dims, jnp.float32) * spread * factor_of
    return jnp.minimum(jnp.maximum(result, -limit), limit).astype(held_as)


def gaussian_with(key, extent, width, bound, shards, heavy, held_as=jnp.bfloat16):
    entries = width * jax.random.normal(key, extent, jnp.float32)
    if shards:
        entries = entries * shard_levels(key, extent, shards, -0.22, 0.18)
    return jnp.clip(spiked(entries, jax.random.fold_in(key, 3), *heavy), -bound, bound).astype(held_as)


def setup_inputs(seed: int = 0) -> dict:
    splits = jax.random.split(jax.random.key(seed), 6)
    tokens = bell_draw(splits[0], (TOKENS, D), 1.0, 6.0, ((0, 256),))
    gate_weight = bell_draw(splits[1], (D, FF), D ** -0.5, 0.125, ((0, 16), (1, 16)))
    up_weight = bell_draw(splits[2], (D, FF), D ** -0.5, 0.125, ((0, 16), (1, 16)))
    down_weight = bell_draw(splits[3], (FF, D), FF ** -0.5, 0.078125, ((0, 16), (1, 16)))
    grad_out = gaussian_with(splits[4], (TOKENS, D), 1.0, 24.0, ((0, 256),), (0, 1, 256, 6.0))
    return {"tokens": tokens, "gate_weight": gate_weight, "up_weight": up_weight, "down_weight": down_weight, "grad_out": grad_out}


def reference(tokens, gate_weight, up_weight, down_weight, grad_out):
    gate_pre = jnp.dot(tokens, gate_weight, preferred_element_type=jnp.float32)
    up_pre = jnp.dot(tokens, up_weight, preferred_element_type=jnp.float32)
    sig_gate = jax.nn.sigmoid(gate_pre)
    active = gate_pre * sig_gate
    hidden = (active * up_pre).astype(jnp.bfloat16)
    d_hidden = jnp.dot(grad_out, down_weight.T, preferred_element_type=jnp.float32)
    d_gate = (d_hidden * up_pre * sig_gate * (1.0 + gate_pre * (1.0 - sig_gate))).astype(jnp.bfloat16)
    d_up = (d_hidden * active).astype(jnp.bfloat16)
    grad_input = (jnp.dot(d_gate, gate_weight.T, preferred_element_type=jnp.float32)
                  + jnp.dot(d_up, up_weight.T, preferred_element_type=jnp.float32)).astype(jnp.bfloat16)
    grad_gate = jnp.dot(tokens.T, d_gate, preferred_element_type=jnp.float32)
    grad_up = jnp.dot(tokens.T, d_up, preferred_element_type=jnp.float32)
    grad_down = jnp.dot(hidden.T, grad_out, preferred_element_type=jnp.float32)
    return grad_input, grad_gate, grad_up, grad_down
```

```python
import jax
import jax.numpy as jnp
from jax import lax
from jax.experimental import pallas as pl
from jax.experimental.pallas import tpu as pltpu
from jax.sharding import Mesh
from jax.sharding import PartitionSpec as P


SIZES = {"y": 4, "x": 4, "z": 8, "core": 2}
BF = jnp.bfloat16
F32 = jnp.float32


def shift(a, axis, by):
    n = SIZES[axis]
    return lax.ppermute(a, axis, [(i, (i + by) % n) for i in range(n)])


def dot(left, right, dims):
    return lax.dot_general(left, right, ((dims[0], dims[1]), ((), ())), preferred_element_type=F32)


def turned(idx, ry, rx):
    return ((idx[0] + ry) & 3) * 4 + ((idx[1] + rx) & 3)


def turn_kernel(idx, a, b, oa, ob):
    for ry in range(4):
        for rx in range(4):
            at = pl.multiple_of(turned(idx, ry, rx) * 128, 128)
            to = (ry * 4 + rx) * 128
            oa[:, to : to + 128] = a[:, pl.ds(at, 128)]
            ob[:, to : to + 128] = b[:, pl.ds(at, 128)]


def turn(idx, a, b):
    shape = jax.ShapeDtypeStruct(a.shape, a.dtype)
    return pl.pallas_call(
        turn_kernel,
        out_shape=(shape, shape),
        in_specs=[pl.BlockSpec(memory_space=pltpu.SMEM)] + [pl.BlockSpec(memory_space=pltpu.VMEM)] * 2,
        out_specs=(pl.BlockSpec(memory_space=pltpu.VMEM),) * 2,
        compiler_params=pltpu.CompilerParams(vmem_limit_bytes=8 * 2**20),
        name="turn",
    )(idx, a, b)


def back_kernel(idx, own, right, left, out):
    for ry in range(4):
        for rx in range(4):
            to = pl.multiple_of(turned(idx, ry, rx) * 128, 128)
            c = slice((ry * 4 + rx) * 128, (ry * 4 + rx + 1) * 128)
            total = own[:, c] + right[:, c].astype(F32) + left[:, c].astype(F32)
            out[:, pl.ds(to, 128)] = total.astype(BF)


def turn_back(idx, own, right, left):
    return pl.pallas_call(
        back_kernel,
        out_shape=jax.ShapeDtypeStruct(own.shape, BF),
        in_specs=[pl.BlockSpec(memory_space=pltpu.SMEM)] + [pl.BlockSpec(memory_space=pltpu.VMEM)] * 3,
        out_specs=pl.BlockSpec(memory_space=pltpu.VMEM),
        compiler_params=pltpu.CompilerParams(vmem_limit_bytes=8 * 2**20),
        name="turn_back",
    )(idx, own, right, left)


def spread(a, axis):
    return [a, shift(a, axis, -1), shift(a, axis, 2), shift(a, axis, 1)]


def gather_weights(w):
    half = w.shape[0] // 2
    first, second = w[:half], w[half:]
    x_all = jnp.concatenate(spread(first, "x"), 0)
    y_all = jnp.concatenate(spread(second, "y"), 0)
    top = spread(x_all, "y")
    low = spread(y_all, "x")
    part = lambda a, k: a[k * half : (k + 1) * half]
    top = jnp.concatenate([part(top[ry], rx) for ry in range(4) for rx in range(4)], 1)
    low = jnp.concatenate([part(low[rx], ry) for ry in range(4) for rx in range(4)], 1)
    return jnp.concatenate([top, low], 0)


def reduce_pieces(pieces, axis):
    got = [shift(pieces[r].astype(BF), axis, r) for r in range(1, 4)]
    return pieces[0] + (got[0].astype(F32) + got[1].astype(F32)) + got[2].astype(F32)


def body(tokens, gate_weight, up_weight, down_weight, grad_out):
    idx = jnp.stack([lax.axis_index("y"), lax.axis_index("x")]).astype(jnp.int32)
    tok, cot = turn(idx, tokens, grad_out)
    toks, cots = {0: tok}, {0: cot}
    r_t, l_t, r_c, l_c = tok, tok, cot, cot
    for k in range(1, 4):
        r_t, l_t = shift(r_t, "z", -1), shift(l_t, "z", 1)
        r_c, l_c = shift(r_c, "z", -1), shift(l_c, "z", 1)
        toks[k], toks[-k], cots[k], cots[-k] = r_t, l_t, r_c, l_c
    toks[4], cots[4] = shift(r_t, "z", -1), shift(l_c, "z", 1)
    w = jnp.concatenate([gate_weight.T, up_weight.T, down_weight], 0)
    mine = gather_weights(w)
    other = shift(mine, "core", 1)
    h = gate_weight.shape[1]
    gate, up, down = (jnp.concatenate([mine[k * h : (k + 1) * h], other[k * h : (k + 1) * h]], 0) for k in range(3))

    def forward(t, c):
        gate_pre = dot(t, gate, ((1,), (1,)))
        up_pre = dot(t, up, ((1,), (1,)))
        sig = jax.nn.sigmoid(gate_pre)
        active = gate_pre * sig
        hidden = (active * up_pre).astype(BF)
        d_hidden = dot(c, down, ((1,), (1,)))
        d_gate = (d_hidden * up_pre * sig * (1.0 + gate_pre * (1.0 - sig))).astype(BF)
        d_up = (d_hidden * active).astype(BF)
        return hidden, d_gate, d_up

    def to_input(d_gate, d_up):
        return dot(d_gate, gate, ((1,), (0,))) + dot(d_up, up, ((1,), (0,)))

    near, far = (0, 1, -1, 2, -2), (3, -3, 4)
    outs = []
    gi = {}
    for group in (near, far):
        t = jnp.concatenate([toks[k] for k in group], 0)
        c = jnp.concatenate([cots[k] for k in group], 0)
        hid, dg, du = forward(t, c)
        part = to_input(dg, du)
        for n, k in enumerate(group):
            gi[k] = part[n * 64 : (n + 1) * 64]
        outs.append((t, c, hid, dg, du))
    t, c, hid, dg, du = (jnp.concatenate(p, 0) for p in zip(*outs))
    d = t.shape[1] // 2
    m_r = shift(gi[4][:, :d].astype(BF), "z", 1)
    m_l = shift(gi[4][:, d:].astype(BF), "z", -1)
    m_r = jnp.concatenate([gi[3][:, :d] + m_r.astype(F32), gi[3][:, d:]], 1).astype(BF)
    m_l = jnp.concatenate([gi[-3][:, :d], gi[-3][:, d:] + m_l.astype(F32)], 1).astype(BF)
    for k in (2, 1):
        m_r, m_l = shift(m_r, "z", 1), shift(m_l, "z", -1)
        m_r = (gi[k] + m_r.astype(F32)).astype(BF)
        m_l = (gi[-k] + m_l.astype(F32)).astype(BF)
    m_r, m_l = shift(m_r, "z", 1), shift(m_l, "z", -1)
    grad_input = turn_back(idx, gi[0], m_r, m_l)

    def weight_grads(cols):
        return [dot(a[:, cols], b, ((0,), (0,))) for a, b in ((dg, t), (du, t), (hid, c))]

    theirs = jnp.concatenate(weight_grads(slice(h, 2 * h)), 0).astype(BF)
    theirs = shift(theirs, "core", 1)
    total = jnp.concatenate(weight_grads(slice(0, h)), 0) + theirs.astype(F32)
    half = total.shape[0] // 2
    top, low = total[:half], total[half:]
    block = lambda a, k: a[:, k * 128 : (k + 1) * 128]
    top = reduce_pieces([jnp.concatenate([block(top, ry * 4 + rx) for ry in range(4)], 1) for rx in range(4)], "x")
    low = reduce_pieces([low[:, ry * 512 : (ry + 1) * 512] for ry in range(4)], "y")
    top = reduce_pieces([block(top, ry) for ry in range(4)], "y")
    low = reduce_pieces([block(low, rx) for rx in range(4)], "x")
    grads = jnp.concatenate([top, low], 0)
    return grad_input, grads[:h].T, grads[h : 2 * h].T, grads[2 * h :]


def solution(mesh):
    fine = Mesh(mesh.devices.reshape(4, 4, 8, 2), ("y", "x", "z", "core"))
    fs, tp = ("y", "x"), ("z", "core")
    rows = P(fs + tp, None)
    in_specs = (rows, P(fs, tp), P(fs, tp), P(tp, fs), rows)
    out_specs = (rows, P(fs, tp), P(fs, tp), P(tp, fs))
    return jax.shard_map(body, mesh=fine, in_specs=in_specs, out_specs=out_specs, check_vma=False)
```

```python
import functools

import jax
import jax.numpy as jnp
from jax import lax
from jax.experimental import pallas as pl
from jax.experimental.pallas import tpu as pltpu
from jax.sharding import Mesh
from jax.sharding import PartitionSpec as P


OFFSET = (0, 1, 3, 2)
SIZES = {"y": 4, "x": 4, "z": 8, "core": 2}
BF = jnp.bfloat16
F32 = jnp.float32
VMEM = pl.BlockSpec(memory_space=pltpu.VMEM)
SMEM = pl.BlockSpec(memory_space=pltpu.SMEM)


def shift(a, axis, by):
    n = SIZES[axis]
    return lax.ppermute(a, axis, [(i, (i + by) % n) for i in range(n)])


def shift_plane(a, first, by):
    pairs = []
    for y in range(4):
        for x in range(4):
            for core in range(2):
                along_x = (core == 0) == first
                to_y, to_x = (y, (x + by) % 4) if along_x else ((y + by) % 4, x)
                pairs.append(((y * 4 + x) * 2 + core, (to_y * 4 + to_x) * 2 + core))
    return lax.ppermute(a, ("y", "x", "core"), pairs)


def dot(left, right, dims):
    return lax.dot_general(left, right, (dims, ((), ())), preferred_element_type=F32)


def place(idx, p, s):
    y, x, core = idx[0], idx[1], idx[2]
    p, s = p ^ (p >> 1), s ^ (s >> 1)
    dy, dx = jnp.where(core == 0, s, p), jnp.where(core == 0, p, s)
    return pl.multiple_of((((y + dy) & 3) * 4 + ((x + dx) & 3)) * 128, 128)


def back_kernel(idx, own, right, left, out):
    for k in range(16):
        c = slice(k * 128, (k + 1) * 128)
        total = own[:, c] + right[:, c].astype(F32) + left[:, c].astype(F32)
        out[:, pl.ds(place(idx, k // 4, k % 4), 128)] = total.astype(BF)


def turn_back(idx, own, right, left):
    return pl.pallas_call(
        back_kernel,
        out_shape=jax.ShapeDtypeStruct(own.shape, BF),
        in_specs=[SMEM, VMEM, VMEM, VMEM],
        out_specs=VMEM,
        compiler_params=pltpu.CompilerParams(vmem_limit_bytes=8 * 2**20),
        name="turn_back",
    )(idx, own, right, left)


def call(kernel, outs, ins, scratch=(), limit=8, scalars=0):
    return pl.pallas_call(
        kernel,
        out_shape=tuple(jax.ShapeDtypeStruct(shape, dtype) for shape, dtype in outs),
        in_specs=[SMEM] * scalars + [VMEM] * (len(ins) - scalars),
        out_specs=(VMEM,) * len(outs),
        scratch_shapes=[pltpu.VMEM(shape, dtype) for shape, dtype in scratch],
        compiler_params=pltpu.CompilerParams(vmem_limit_bytes=limit * 2**20),
    )(*ins)


def lanes(k, n=128):
    return slice(k * n, (k + 1) * n)


def assemble_kernel(*refs):
    first, mine, send = refs[:3], refs[3], refs[4]
    n = mine.shape[0]

    def step(s, carry):
        for p in range(3):
            block = first[p][pl.ds(pl.multiple_of(s * n, 32), n)]
            mine[:, pl.ds(pl.multiple_of(s * 128 + p * 512, 128), 128)] = block
            send[:, pl.ds(pl.multiple_of(s * 384 + p * 128, 128), 128)] = block
        return carry

    lax.fori_loop(0, 4, step, 0)


def last_kernel(up, down, mine):
    n = mine.shape[0]
    for s in range(4):
        mine[:, lanes(s)] = (up if s < 2 else down)[(s % 2) * n : (s % 2 + 1) * n]


def weights_of(refs, rows, core):
    return jnp.concatenate([ref[rows] for ref in refs[2 * core : 2 * core + 2]], 1)


def theirs_order(a):
    most = [a[:, s * 512 : s * 512 + 384] for s in range(4)]
    return jnp.concatenate(most + [a[:, s * 512 + 384 : (s + 1) * 512] for s in range(4)], 1)


def forward_kernel(idx, *refs):
    blocks, w, (held, *outs) = refs[:16], refs[16:20], refs[20:]

    def turn(k, carry):
        at = pl.ds(place(idx, k >> 2, k & 3), 128)
        to = pl.ds(pl.multiple_of(k * 128, 128), 128)
        for m in range(16):
            held[m * 64 : m * 64 + 64, to] = blocks[m][:, at]
        return carry

    lax.fori_loop(0, 16, turn, 0)
    h = w[0].shape[0] // 3

    def half(n, carry):
        to = pl.ds(pl.multiple_of(n * 256, 256), 256)
        tok, cot = held[to], held[pl.ds(pl.multiple_of(512 + n * 256, 256), 256)]
        for core in range(2):
            d_pre, hid = outs[core], outs[core + 2]
            if core:
                tok, cot = theirs_order(tok), theirs_order(cot)
            pre = dot(weights_of(w, slice(0, 2 * h), core), tok, ((1,), (1,)))
            d_hidden = dot(weights_of(w, slice(2 * h, 3 * h), core), cot, ((1,), (1,)))
            gate_pre, up_pre = pre[:h], pre[h:]
            sig = jax.nn.sigmoid(gate_pre)
            active = gate_pre * sig
            hid[:, to] = (active * up_pre).astype(BF)
            d_pre[:h, to] = (d_hidden * up_pre * sig * (1.0 + gate_pre * (1.0 - sig))).astype(BF)
            d_pre[h:, to] = (d_hidden * active).astype(BF)
        return carry

    lax.fori_loop(0, 2, half, 0)


def forward(idx, toks, cots, w):
    d, h = 2048, w[0].shape[0] // 3
    outs = [((1024, d), BF)] + [((2 * h, 512), BF)] * 2 + [((h, 512), BF)] * 2
    return call(forward_kernel, outs, (idx, *toks, *cots, *w), limit=16, scalars=1)


def input_kernel(d_mine, d_other, m_most, m_last, o_most, o_last, *refs, half):
    outs, (a, b) = refs[:-2], refs[-2:]
    a[...] = d_mine[:, lanes(half, 256)].T
    b[...] = d_other[:, lanes(half, 256)].T
    n = d_mine.shape[0]

    def cols(start, width=256):
        return pl.ds(pl.multiple_of(start, 128), width)

    def one(p, k, mine):
        if k:
            other = jnp.concatenate([o_most[:n, cols(p * 384 + 256, 128)], o_last[:n, cols(p * 128, 128)]], 1)
        else:
            other = o_most[:n, cols(p * 384)]
        part = dot(a[...], mine, ((1,), (0,))) + dot(b[...], other, ((1,), (0,)))
        for m, out in enumerate(outs):
            out[:, cols(p * 512 + k * 256)] = part[m * 64 : m * 64 + 64].astype(out.dtype)

    def step(p, carry):
        for k in range(2):
            one(p, k, m_most[:n, cols(p * 512 + k * 256)])
        return carry

    lax.fori_loop(0, 3, step, 0)
    for k in range(2):
        one(3, k, m_last[:n, lanes(k, 256)])


def to_input(d_mine, d_other, w, half, types):
    d, n = 2048, d_mine.shape[0]
    outs = [((64, d), dtype) for dtype in types]
    kernel = functools.partial(input_kernel, half=half)
    return call(kernel, outs, (d_mine, d_other, *w), [((256, n), BF)] * 2, 16)


def grads_at(at, d, h, held):
    dims = ((1,), (0,))
    cols = lambda rows: jnp.concatenate([held[rows, c] for c in at], 1)
    return dot(d[...], cols(slice(0, 512)), dims), dot(h[...], cols(slice(512, 1024)), dims)


def theirs_kernel(d, h, held, out, *, pair):
    n = d.shape[0]

    def step(k, carry):
        at = [pl.ds(pl.multiple_of(k * 1024 + s * 512 + pair * 128, 128), 256) for s in range(2)]
        top, low = grads_at(at, d, h, held)
        for m in range(2):
            for s in range(2):
                to, of = pl.ds(pl.multiple_of(m * 512 + k * 256 + s * 128, 128), 128), lanes(2 * s + m)
                out[:n, to] = top[:, of].astype(BF)
                out[n:, to] = low[:, of].astype(BF)
        return carry

    if pair:
        for k in range(2):
            step(k, 0)
    else:
        lax.fori_loop(0, 2, step, 0)


def own_kernel(d, h, held, theirs, *outs, pair):
    n = d.shape[0]

    for m in range(2):

        def step(k, carry, m=m, width=512 if pair else 256):
            col = lambda base: pl.ds(pl.multiple_of(base + k * width, 256), width)
            top, low = grads_at([col((pair + m) * 512)], d, h, held)
            outs[m][:n, col(0)] = (top + theirs[:n, col(m * 512)].astype(F32)).astype(outs[m].dtype)
            outs[m][n:, col(0)] = (low + theirs[n:, col(m * 512)].astype(F32)).astype(outs[m].dtype)
            return carry

        lax.fori_loop(0, 1 if pair else 2, step, 0)


def theirs_grads(ins, pair):
    n = ins[0].shape[0] + ins[1].shape[0]
    return call(functools.partial(theirs_kernel, pair=pair), [((n, 1024), BF)], ins, limit=16)[0]


def own_grads(ins, theirs, pair):
    n = ins[0].shape[0] + ins[1].shape[0]
    outs = [((n, 512), F32 if pair + m == 0 else BF) for m in range(2)]
    return call(functools.partial(own_kernel, pair=pair), outs, (*ins, theirs), limit=20)


def sum_kernel(own, r1, r2, r3, keep, *outs):
    def step(k, carry):
        rows = pl.ds(pl.multiple_of(k * 352, 32), 352)
        total = own[rows] + (r1[rows].astype(F32) + r2[rows].astype(F32)) + r3[rows].astype(F32)
        keep[rows] = total[:, :128]
        for s, out in enumerate(outs):
            out[rows] = total[:, lanes(s + 1)].astype(BF)
        return carry

    lax.fori_loop(0, 3, step, 0)


def add_kernel(own, got, out):
    out[...] = (own[...] + got[...].astype(F32)).astype(BF)


def add(own, got):
    return call(add_kernel, [(own.shape, BF)], (own, got))[0]


def spread(a, first):
    return [a] + [shift_plane(a, first, -OFFSET[q]) for q in (1, 2, 3)]


def inner(tokens, gate_weight, up_weight, down_weight, grad_out):
    idx = jnp.stack([lax.axis_index(a) for a in ("y", "x", "core")]).astype(jnp.int32)
    h = gate_weight.shape[1]
    w = jnp.concatenate([gate_weight.T, up_weight.T, down_weight], 0)
    n = w.shape[0]
    ring = jnp.concatenate(spread(w, False), 0)
    up, down = shift_plane(ring, True, -1), shift_plane(ring, True, 1)
    m_most, send = call(assemble_kernel, [((n, 1536), BF)] * 2, (ring, up, down))
    up, down = shift_plane(up[: 2 * n], True, -1), shift_plane(down[2 * n :], True, 1)
    (m_last,) = call(last_kernel, [((n, 512), BF)], (up, down))
    weights = (m_most, m_last, shift(send, "core", 1), shift(m_last, "core", 1))

    toks, cots = {0: tokens}, {0: grad_out}
    for k in range(1, 4):
        for held in (toks, cots):
            held[k] = shift(held[k - 1], "z", -1)
            held[-k] = shift(held[1 - k], "z", 1)
    toks[4], cots[4] = shift(toks[3], "z", -1), shift(cots[-3], "z", 1)

    ring = (0, 1, -1, 2, -2, 3, -3, 4)
    held, dm, do, hm, ho = forward(idx, [toks[k] for k in ring], [cots[k] for k in ring], weights)
    far = to_input(dm, do, weights, 1, [F32] * 2 + [BF] * 2)
    gi = dict(zip(ring, [*to_input(dm, do, weights, 0, [F32] * 4), *far]))

    m_r, m_l = add(gi[3], shift(gi[4], "z", 1)), gi[-3]
    for k in (2, 1):
        m_r, m_l = shift(m_r, "z", 1), shift(m_l, "z", -1)
        m_r, m_l = add(gi[k], m_r), add(gi[-k], m_l)
    m_r, m_l = shift(m_r, "z", 1), shift(m_l, "z", -1)
    grad_input = turn_back(idx, gi[0], m_r, m_l)

    theirs_ins = (do, ho, held)
    own_ins = (dm, hm, held)
    sent = [theirs_grads(theirs_ins, pair) for pair in (2, 0)]
    got = [shift(a, "core", 1) for a in sent]
    (p2, p3), (p0, p1) = (own_grads(own_ins, a, pair) for a, pair in zip(got, (2, 0)))
    r = [shift_plane(a, True, OFFSET[q]) for q, a in ((1, p1), (2, p2), (3, p3))]
    keep, *sends = call(sum_kernel, [((n, 128), F32)] + [((n, 128), BF)] * 3, (p0, *r), limit=4)
    r = [shift_plane(a, False, OFFSET[q + 1]) for q, a in enumerate(sends)]
    grads = keep + (r[0].astype(F32) + r[1].astype(F32)) + r[2].astype(F32)
    return grad_input, grads[:h].T, grads[h : 2 * h].T, grads[2 * h :]


def solution(mesh):
    fine = Mesh(mesh.devices.reshape(4, 4, 8, 2), ("y", "x", "z", "core"))
    fs, tp = ("y", "x"), ("z", "core")
    rows = P(fs + tp, None)
    in_specs = (rows, P(fs, tp), P(fs, tp), P(tp, fs), rows)
    out_specs = (rows, P(fs, tp), P(fs, tp), P(tp, fs))
    return jax.shard_map(inner, mesh=fine, in_specs=in_specs, out_specs=out_specs, check_vma=False)
```
